32 devices in a mesh: sp: 16 (over z, y, x), tp: 2 (over core).
Axes of the slice: x: 2, y: 2, z: 4, core: 2. Of those that a mesh axis runs over, the one named last changes fastest.
Arguments:
- moe_in: bfloat16 [3072, 2048], P('sp'), may hold values from -72 to 72
- cotangent: bfloat16 [3072, 2048], P('sp'), may hold values from -6 to 6
- route_ids: int32 [3072, 2], P('sp'), may hold values from 0 to 15, all different within a row; in each aligned block of 192 rows (0 to 191, 192 to 383, ...) at most 36 rows name the same one
- route_weights: float32 [3072, 2], P('sp'), may hold values from 0.1 to 0.9
- gate_weight: bfloat16 [16, 2048, 1536], P('sp', None, 'tp'), may hold values from -0.125 to 0.125
- up_weight: bfloat16 [16, 2048, 1536], P('sp', None, 'tp'), may hold values from -0.125 to 0.125
- down_weight: bfloat16 [16, 1536, 2048], P('sp', 'tp'), may hold values from -0.15625 to 0.15625
- out_weight: bfloat16 [2048, 1024], P(None, 'tp'), may hold values from -0.1875 to 0.1875
- query: bfloat16 [3072, 512], P('sp', 'tp'), may hold values from -6 to 6
- key_in: bfloat16 [3072, 512], P('sp', 'tp'), may hold values from -0.119628906 to 0.119628906
- value: bfloat16 [3072, 1024], P('sp', 'tp'), may hold values from -6 to 6
- log_decay: float32 [3072, 512], P('sp', 'tp'), may hold values from -1 to 0
Outputs:
- grad_gate: bfloat16 [16, 2048, 1536], P('sp', None, 'tp')
- grad_up: bfloat16 [16, 2048, 1536], P('sp', None, 'tp')
- grad_down: bfloat16 [16, 1536, 2048], P('sp', 'tp')
- grad_out: float32 [2048, 1024], P('sp', 'tp')
- grad_query: float32 [3072, 512], P('sp', 'tp')
- grad_key: float32 [3072, 512], P('sp', 'tp')
- grad_value: float32 [3072, 1024], P('sp', 'tp')
- grad_decay: float32 [3072, 512], P('sp', 'tp')
The draws below stay inside these ranges and needn't reach their ends.
Inputs may be any that keep to these rules, and one draw needn't show every extreme that they name: `route_ids`: in every aligned block of 192 rows no expert is named by more than 36 rows, a bound that some block reaches; the numbers of a row differ.
All inputs are finite; a program needn't handle non-finite values.
Results may differ from the reference program's by a relative error of at most 0.022.
Values may be sent and summed in bfloat16 or wider, within the bound.
No kernel may reach another device: no remote copies, remote signals or barrier semaphores. Data moves between devices by JAX's collectives and lax.ppermute only.
A program may use at most 128 MiB of HBM per device.

```python
import math
import jax
import jax.numpy as jnp
import numpy as np
from jax import lax

D = 2048
FF = 1536
H = 4
DK = 128
DV = 256
BLK = 64
TOP = 2
TOK_DEV = 192
SEQUENCE_TOKENS = 3072
EXPERTS = 16
CAP = 36
FF_DEV = 768
N_SP = 16
N_TP = 2


def draw_moe_in(key, part):
    key_base = jax.random.fold_in(key, 11)
    key_rows = jax.random.fold_in(key, 12)
    normal_part = jnp.clip(jax.random.normal(key_base, (SEQUENCE_TOKENS, D), jnp.float32), -6.0, 6.0)
    top_scale = math.log(3.0)
    row_scale = jnp.exp(jax.random.uniform(key_rows, (SEQUENCE_TOKENS, 1), jnp.float32, 0.0, top_scale))
    return (normal_part * row_scale).astype(jnp.bfloat16)


def draw_log_decay(key, part):
    key_kind = jax.random.fold_in(key, 21)
    key_fast = jax.random.fold_in(key, 22)
    key_slow = jax.random.fold_in(key, 23)
    key_span = jax.random.fold_in(key, 24)
    key_rough = jax.random.fold_in(key, 25)
    key_location = jax.random.fold_in(key, 26)
    key_magnitude = jax.random.fold_in(key, 27)
    fast_share = 0.5
    channels = H * DK
    is_fast = jax.random.uniform(key_kind, (channels,), jnp.float32) < fast_share
    fast_rate = jnp.exp(jax.random.uniform(key_fast, (channels,), jnp.float32, math.log(0.01), math.log(1.0 / 30.0)))
    slow_rate = jnp.exp(jax.random.uniform(key_slow, (channels,), jnp.float32, math.log(0.1), 0.0)) * (0.4 / SEQUENCE_TOKENS)
    decay_speed = jnp.where(is_fast, fast_rate, slow_rate)
    extent_multiplier = jnp.exp(jax.random.uniform(key_span, (SEQUENCE_TOKENS // TOK_DEV,), jnp.float32, math.log(0.5), math.log(2.0)))
    extent_multiplier = jnp.repeat(extent_multiplier, TOK_DEV)[:, None]
    noise_level = jax.random.uniform(key_rough, (SEQUENCE_TOKENS, channels), jnp.float32, 0.5, 1.5)
    spike_position = jax.random.randint(key_location, (2,), 0, SEQUENCE_TOKENS)
    spike_magnitude = jax.random.uniform(key_magnitude, (2,), jnp.float32, 0.22, 0.69)
    token_positions = jnp.arange(SEQUENCE_TOKENS)[:, None]
    spike_value = jnp.sum(jnp.where(token_positions == spike_position[None, :], spike_magnitude[None, :], 0.0), axis=1)
    return -(decay_speed[None, :] * extent_multiplier * noise_level) - spike_value[:, None]


def spiked(drawn, own_key, source, target, blocks, factor):
    owner, partner = [(jnp.arange(drawn.shape[position]) // (drawn.shape[position] // blocks)).reshape([-1 if axis == position else 1 for axis in range(drawn.ndim)]) for position in (source, target)]
    chosen = jax.random.permutation(own_key, blocks)[partner]
    strong = (owner == chosen) | (owner == (partner + blocks // 2) % blocks)
    return jnp.where(strong, factor * drawn, drawn)


def steps_of(rng, dims, pieces, smallest, high):
    loudness, own = 1.0, jax.random.fold_in(rng, 6)
    for dim, shards_of in pieces:
        steps = jnp.exp(jax.random.uniform(jax.random.fold_in(own, dim), (shards_of,), jnp.float32, smallest / len(pieces), high / len(pieces)))
        loudness = loudness * jnp.repeat(steps, dims[dim] // shards_of).reshape([-1 if axis == dim else 1 for axis in range(len(dims))])
    return loudness


def shared_out(key, own, number, rows, count, top, most, skew):
    ranking = jax.random.permutation(key, count)
    packed, ordinary = shares(count, rows * top, most, skew, True), shares(count, rows * top, most, skew, False)
    places = jnp.arange(count)

    def named(sizes, offset_by):
        used = int((sizes > 0).sum())
        fixed = max(1, used // 4)
        shifted = fixed + (places - fixed + offset_by * (used - fixed)) % max(1, count - fixed)
        return jnp.zeros((count,), jnp.int32).at[ranking[jnp.where(places < fixed, places, shifted)]].set(jnp.asarray(sizes, jnp.int32))

    sizes = jnp.where(number % 4 == 0, named(packed, number // 4), named(ordinary, number - number // 4 - 1))
    mixed = jax.random.permutation(jax.random.fold_in(own, 3), count)
    source_of, sink = mixed[0:count // 2 * 2:2], mixed[1:count // 2 * 2:2]
    room = jnp.minimum(sizes[source_of] - 1, most - sizes[sink]) // 2
    room = jnp.where((source_of == ranking[0]) | (sink == ranking[0]) | (sizes[sink] == 0), 0, jnp.maximum(room, 0))
    shifted = jax.random.randint(jax.random.fold_in(own, 4), (count // 2,), 0, 1 << 20) % (room + 1)
    sizes = sizes.at[source_of].add(-shifted).at[sink].add(shifted)
    labels = jnp.searchsorted(jnp.cumsum(sizes), jnp.arange(rows * top), side="right").astype(jnp.int32)
    table = labels.reshape(top, rows).T
    table = table[jax.random.permutation(jax.random.fold_in(own, 1), rows)]
    offset_by = jax.random.randint(jax.random.fold_in(own, 2), (rows, 1), 0, top)
    return jnp.take_along_axis(table, (jnp.arange(top)[None, :] + offset_by) % top, axis=1)


def shares(amount, total, bound, skew, full):
    loads = [(1 << 20) // math.isqrt(standing ** skew) + 1 for standing in range(1, amount + 1)]
    largest = bound if full else min(bound, max(-(-total // amount), total * loads[0] // sum(loads)))
    least = 1 if total - largest >= amount - 1 else 0
    given, surplus = [largest] + [least] * (amount - 1), total - largest - least * (amount - 1)
    while surplus > 0:
        candidates = [i for i in range(1, amount) if given[i] < largest] or [i for i in range(1, amount) if given[i] < bound]
        whole, budget = sum([loads[i] for i in candidates]), surplus
        for i in candidates:
            more = min(bound - given[i], max(1, budget * loads[i] // whole), surplus)
            given[i] = given[i] + more
            surplus = surplus - more
    return np.array(given)


def normal_values(rng, dims, scale, most, split=(), kind=jnp.bfloat16):
    entries = scale * jax.random.normal(rng, dims, jnp.float32)
    if split:
        entries = entries * steps_of(rng, dims, split, -0.22, 0.18)
    return jnp.clip(entries, -most, most).astype(kind)


def gaussian_with(own_key, shape, width, limit, split, heavy, held_as=jnp.bfloat16):
    entries = width * jax.random.normal(own_key, shape, jnp.float32)
    if split:
        entries = entries * steps_of(own_key, shape, split, -0.22, 0.18)
    return jnp.clip(spiked(entries, jax.random.fold_in(own_key, 3), *heavy), -limit, limit).astype(held_as)


def setup_inputs(seed: int = 0) -> dict:
    key_of = jax.random.split(jax.random.key(seed), 13)
    moe_in = draw_moe_in(jax.random.fold_in(key_of[12], 71), 0)
    cotangent = gaussian_with(key_of[1], (SEQUENCE_TOKENS, D), 1.0, 6.0, ((0, 16),), (0, 1, 16, 2.0))
    route_ids_keys = jax.random.split(jax.random.fold_in(key_of[2], 1), SEQUENCE_TOKENS // TOK_DEV)
    route_ids_turns = jax.random.permutation(jax.random.fold_in(key_of[2], 3), SEQUENCE_TOKENS // TOK_DEV)
    route_ids = jax.vmap(lambda own, number: shared_out(jax.random.fold_in(key_of[2], 2), own, number, TOK_DEV, EXPERTS, TOP, CAP, 1))(route_ids_keys, route_ids_turns).reshape((SEQUENCE_TOKENS, TOP))
    route_weights = jnp.clip(0.1 + 0.79999997 * jax.random.uniform(key_of[3], (SEQUENCE_TOKENS, TOP), jnp.float32) ** steps_of(key_of[3], (SEQUENCE_TOKENS, TOP), ((0, 16),), -0.2, 0.2), 0.1, 0.9)
    gate_weight = normal_values(key_of[4], (EXPERTS, D, FF), D ** -0.5, 0.125, ((0, 16), (2, 2)))
    up_weight = normal_values(key_of[5], (EXPERTS, D, FF), D ** -0.5, 0.125, ((0, 16), (2, 2)))
    down_weight = normal_values(key_of[6], (EXPERTS, FF, D), FF ** -0.5, 0.15625, ((0, 16), (1, 2)))
    out_weight = normal_values(key_of[7], (D, H * DV), (H * DV) ** -0.5, 0.1875, ((1, 2),))
    query = normal_values(key_of[8], (SEQUENCE_TOKENS, H * DK), 1.0, 6.0, ((0, 16), (1, 2)))
    key_in = normal_values(key_of[9], (SEQUENCE_TOKENS, H * DK), 0.02, 0.119628906, ((0, 16), (1, 2)))
    value = normal_values(key_of[10], (SEQUENCE_TOKENS, H * DV), 1.0, 6.0, ((0, 16), (1, 2)))
    log_decay = draw_log_decay(jax.random.fold_in(key_of[12], 71), 0)
    return {"moe_in": moe_in, "cotangent": cotangent, "route_ids": route_ids, "route_weights": route_weights, "gate_weight": gate_weight, "up_weight": up_weight, "down_weight": down_weight, "out_weight": out_weight, "query": query, "key_in": key_in, "value": value, "log_decay": log_decay}


CLAMP_LIMIT = 7.0
SWISH_ALPHA = 1.702
HIGHEST_PREC = lax.Precision.HIGHEST

def inner_rows(left, right):
    return lax.dot_general(left, right, (((0,), (0,)), ((), ())), preferred_element_type=jnp.float32)

def outer_cols(left, right):
    return lax.dot_general(left, right, (((1,), (1,)), ((), ())), preferred_element_type=jnp.float32)

def route_slots(route_ids):
    flat_ids = route_ids.reshape(N_SP, TOK_DEV * TOP)
    chosen = (flat_ids[:, :, None] == jnp.arange(EXPERTS, dtype=jnp.int32)[None, None, :]).astype(jnp.int32)
    places = lax.optimization_barrier(jnp.sum((jnp.cumsum(chosen, axis=1) - chosen) * chosen, axis=2))
    source = jnp.arange(N_SP, dtype=jnp.int32)[:, None]
    return (flat_ids * (N_SP * CAP) + source * CAP + places).reshape(-1).astype(jnp.int32)

def expert_grads(operands):
    tok_rows, cot_rows, w_gate, w_up, w_down = operands
    pre_gate = jnp.dot(tok_rows, w_gate, preferred_element_type=jnp.float32)
    pre_up = jnp.dot(tok_rows, w_up, preferred_element_type=jnp.float32)
    gate_clamped = jnp.minimum(pre_gate, CLAMP_LIMIT)
    up_clamped = jnp.clip(pre_up, -CLAMP_LIMIT, CLAMP_LIMIT)
    sigmoid_gate = jax.nn.sigmoid(SWISH_ALPHA * gate_clamped)
    activated = ((up_clamped + 1.0) * gate_clamped * sigmoid_gate).astype(jnp.bfloat16)
    grad_down = inner_rows(activated, cot_rows).astype(jnp.bfloat16)
    grad_act = outer_cols(cot_rows, w_down)
    slope = (up_clamped + 1.0) * sigmoid_gate * (1.0 + SWISH_ALPHA * gate_clamped * (1.0 - sigmoid_gate))
    grad_pre_gate = jnp.where(pre_gate < CLAMP_LIMIT, grad_act * slope, 0.0).astype(jnp.bfloat16)
    grad_pre_up = jnp.where(jnp.abs(pre_up) < CLAMP_LIMIT, grad_act * gate_clamped * sigmoid_gate, 0.0).astype(jnp.bfloat16)
    grad_wg = inner_rows(tok_rows, grad_pre_gate).astype(jnp.bfloat16)
    grad_wu = inner_rows(tok_rows, grad_pre_up).astype(jnp.bfloat16)
    returned = jnp.zeros(tok_rows.shape, jnp.float32)
    for ff_piece in range(N_TP):
        offset = ff_piece * FF_DEV
        piece_term = outer_cols(grad_pre_gate[:, offset:offset + FF_DEV], w_gate[:, offset:offset + FF_DEV])
        piece_term = piece_term + outer_cols(grad_pre_up[:, offset:offset + FF_DEV], w_up[:, offset:offset + FF_DEV])
        returned = returned + piece_term.astype(jnp.bfloat16).astype(jnp.float32)
    return (grad_wg, grad_wu, grad_down, returned)

def blocks(array, channels):
    head_count = array.shape[1] // channels
    return array.reshape(-1, BLK, head_count, channels).transpose(0, 2, 1, 3)

def gla_forward(query_f, key_f, value_f, decay_f):
    head_count = query_f.shape[1] // DK
    scaled_q = blocks(query_f * DK ** (-0.5), DK)
    keys_b = blocks(key_f, DK)
    values_b = blocks(value_f, DV)
    log_cum = jnp.cumsum(blocks(decay_f, DK), axis=2)
    log_last = log_cum[:, :, -1:, :]
    q_dec = scaled_q * jnp.exp(log_cum)
    k_grow = keys_b * jnp.exp(-log_cum)
    k_end = keys_b * jnp.exp(log_last - log_cum)
    lower = jnp.tril(jnp.ones((BLK, BLK), jnp.float32))
    scores = jnp.einsum('nhid,nhjd->nhij', q_dec, k_grow, precision=HIGHEST_PREC) * lower
    block_adds = jnp.einsum('nhcd,nhce->nhde', k_end, values_b, precision=HIGHEST_PREC)
    block_fade = jnp.exp(log_last[:, :, 0, :])

    def forward_step(state, inputs):
        fade_n, add_n = inputs
        return (fade_n[..., None] * state + add_n, state)
    start_state = jnp.zeros((head_count, DK, DV), jnp.float32)
    _, starts = lax.scan(forward_step, start_state, (block_fade, block_adds))
    mixer_out = jnp.einsum('nhid,nhde->nhie', q_dec, starts, precision=HIGHEST_PREC)
    mixer_out = mixer_out + jnp.einsum('nhij,nhje->nhie', scores, values_b, precision=HIGHEST_PREC)
    return mixer_out.transpose(0, 2, 1, 3).reshape(-1, head_count * DV)

def reference(moe_in, cotangent, route_ids, route_weights, gate_weight, up_weight, down_weight, out_weight, query, key_in, value, log_decay):
    slot_index = route_slots(route_ids)
    total_slots = EXPERTS * N_SP * CAP
    spread = jnp.repeat(moe_in, TOP, axis=0)
    scaled = (route_weights[:, :, None] * cotangent[:, None, :].astype(jnp.float32)).astype(jnp.bfloat16).reshape(-1, D)
    tok_buffer = jnp.zeros((total_slots, D), jnp.bfloat16).at[slot_index].set(spread).reshape(EXPERTS, N_SP * CAP, D)
    cot_buffer = jnp.zeros((total_slots, D), jnp.bfloat16).at[slot_index].set(scaled).reshape(EXPERTS, N_SP * CAP, D)
    grad_gate, grad_up, grad_down, returned = lax.map(expert_grads, (tok_buffer, cot_buffer, gate_weight, up_weight, down_weight))
    gathered = returned.reshape(total_slots, D)[slot_index].reshape(-1, TOP, D)
    grad_tokens = (cotangent.astype(jnp.float32) + lax.optimization_barrier(jnp.sum(gathered, axis=1))).astype(jnp.bfloat16)
    mixer_cot = jnp.dot(grad_tokens, out_weight, preferred_element_type=jnp.float32)
    mixer_out, pullback = jax.vjp(gla_forward, query.astype(jnp.float32), key_in.astype(jnp.float32), value.astype(jnp.float32), log_decay)
    mixed = mixer_out.astype(jnp.bfloat16)
    grad_out = inner_rows(grad_tokens, mixed)
    grad_query, grad_key, grad_value, grad_decay = pullback(mixer_cot)
    return (grad_gate, grad_up, grad_down, grad_out, grad_query, grad_key, grad_value, grad_decay)
```

```python
import jax
import jax.numpy as jnp
from jax import lax
from jax.experimental import pallas as pl
from jax.experimental.pallas import tpu as pltpu
from jax.sharding import PartitionSpec as P

DK = 128
DV = 256
BLK = 64
TOP = 2
GROUP = 4
LANES = 128

CLAMP_LIMIT = 7.0
SWISH_ALPHA = 1.702
HIGHEST_PREC = lax.Precision.HIGHEST
F32 = jnp.float32
BF16 = jnp.bfloat16


def dot_nn(left, right, precision=None):
    return lax.dot_general(
        left, right, (((1,), (0,)), ((), ())), precision=precision, preferred_element_type=F32
    )


def dot_tn(left, right, precision=None):
    return lax.dot_general(
        left, right, (((0,), (0,)), ((), ())), precision=precision, preferred_element_type=F32
    )


def dot_nt(left, right, precision=None):
    return lax.dot_general(
        left, right, (((1,), (1,)), ((), ())), precision=precision, preferred_element_type=F32
    )


def call(kernel, out_shape, scratch=(), flops=10**8, nbytes=4 * 10**6):
    return pl.pallas_call(
        kernel,
        out_shape=out_shape,
        scratch_shapes=list(scratch),
        cost_estimate=pl.CostEstimate(flops=flops, bytes_accessed=nbytes, transcendentals=0),
    )


def shape(dims, dtype):
    return jax.ShapeDtypeStruct(tuple(dims), dtype)


def route_columns(ids_ref, stride):
    tokens = ids_ref.shape[0]
    ids = ids_ref[...]
    lane = lax.broadcasted_iota(jnp.int32, (tokens, LANES), 1)
    row = lax.broadcasted_iota(jnp.int32, (tokens, tokens), 0)
    col = lax.broadcasted_iota(jnp.int32, (tokens, tokens), 1)
    before = jnp.where(col < row, 1.0, 0.0).astype(BF16)
    slots = []
    base = jnp.zeros((1, LANES), F32)
    for choice in range(TOP):
        own = ids[:, choice : choice + 1]
        named = jnp.where(lane == own, 1.0, 0.0)
        ahead = dot_nn(before, named.astype(BF16)) + base
        place = jnp.sum(named * ahead, axis=1, keepdims=True).astype(jnp.int32)
        slots.append(own * stride + place)
        base = base + jnp.sum(named, axis=0, keepdims=True)
    return slots


def one_hot(slot, start, width):
    lane = lax.broadcasted_iota(jnp.int32, (slot.shape[0], width), 1) + start
    return jnp.where(lane == slot, 1.0, 0.0).astype(BF16)


def lower_ones():
    row = lax.broadcasted_iota(jnp.int32, (BLK, BLK), 0)
    col = lax.broadcasted_iota(jnp.int32, (BLK, BLK), 1)
    return jnp.where(col <= row, 1.0, 0.0)


def log_sums(decay_ref, head, block, lower):
    part = decay_ref[block * BLK : (block + 1) * BLK, head * DK : (head + 1) * DK]
    log_cum = dot_nn(lower, part, HIGHEST_PREC)
    return log_cum, log_cum[BLK - 1 : BLK, :]


def cut(ref, head, block, channels):
    return ref[
        block * BLK : (block + 1) * BLK, head * channels : (head + 1) * channels
    ].astype(F32)


def log_between(logs, first, last):
    row = lax.broadcasted_iota(jnp.int32, logs.shape, 0)
    inside = (row >= first) & (row < last)
    return jnp.exp(jnp.sum(jnp.where(inside, logs, 0.0), axis=0, keepdims=True))


def send_tokens_kernel(
    count, stride, srow, ids_ref, moe_ref, key_ref, value_ref, decay_ref, out_ref, log_ref, state_ref, tile_ref
):
    half = out_ref.shape[1]
    start = pl.multiple_of(lax.axis_index("tp") * half, LANES)
    slots = route_columns(ids_ref, stride)
    tokens = moe_ref[:, pl.ds(start, half)]
    for piece in range(count * stride // LANES):
        first = piece * LANES
        chosen = one_hot(slots[0], first, LANES) + one_hot(slots[1], first, LANES)
        out_ref[first : first + LANES, :] = dot_tn(chosen, tokens).astype(BF16)
    lower = lower_ones()
    heads = key_ref.shape[1] // DK
    spans = key_ref.shape[0] // BLK
    for head in range(heads):
        state = None
        total = None
        for block in range(spans):
            log_cum, last = log_sums(decay_ref, head, block, lower)
            k_end = cut(key_ref, head, block, DK) * jnp.exp(last - log_cum)
            add = dot_tn(cut(value_ref, head, block, DV), k_end, HIGHEST_PREC)
            state = add if state is None else jnp.exp(last) * state + add
            total = last if total is None else total + last
        state_ref[head * DV : (head + 1) * DV, :] = state
        log_ref[:, head * DK : (head + 1) * DK] = total
    rows = state_ref.shape[0] // count
    tile_ref[...] = jnp.zeros_like(tile_ref)
    for chunk in range(count):
        for part in range(half // LANES):
            first = chunk * rows + part * srow
            tile_ref[8 - srow : 8, part * LANES : (part + 1) * LANES] = state_ref[
                first : first + srow, :
            ]
        end = (chunk + 1) * stride
        out_ref[end - 8 : end, :] = (out_ref[end - 8 : end, :].astype(F32) + tile_ref[...]).astype(BF16)


def send_cots_kernel(
    count, stride, srow, ids_ref, weight_ref, cot_ref, tail_ref, logs_ref, out_ref
):
    half = out_ref.shape[1]
    start = pl.multiple_of(lax.axis_index("tp") * half, LANES)
    slots = route_columns(ids_ref, stride)
    cots = cot_ref[:, pl.ds(start, half)].astype(F32)
    weights = weight_ref[...]
    scaled = [(weights[:, c : c + 1] * cots).astype(BF16) for c in range(TOP)]
    for piece in range(count * stride // LANES):
        first = piece * LANES
        rows = dot_tn(one_hot(slots[0], first, LANES), scaled[0])
        rows = rows + dot_tn(one_hot(slots[1], first, LANES), scaled[1])
        out_ref[first : first + LANES, :] = rows.astype(BF16)
    heads = logs_ref.shape[1] // DK
    head = lax.axis_index("sp") * heads // count
    logs = logs_ref[:, pl.ds(pl.multiple_of(head * DK, LANES), DK)]
    fades = jnp.exp(logs)
    kept = lax.broadcasted_iota(jnp.int32, (8, half), 0) >= 8 - srow
    state = jnp.zeros((8, half), F32)
    for span in range(count):
        end = (span + 1) * stride
        out_ref[end - 8 : end, :] = (out_ref[end - 8 : end, :].astype(F32) + state).astype(BF16)
        fade = jnp.concatenate([fades[span : span + 1, :]] * (half // DK), axis=1)
        state = fade * state + jnp.where(kept, tail_ref[span].astype(F32), 0.0)


def mixed_kernel(
    count, srow, query_ref, key_ref, value_ref, decay_ref, tail_ref, mixed_ref, entry_ref, tile_ref
):
    half = tail_ref.shape[2]
    rows = entry_ref.shape[0] // count
    for chunk in range(count):
        tile_ref[...] = tail_ref[chunk].astype(F32)
        for part in range(half // LANES):
            first = chunk * rows + part * srow
            entry_ref[first : first + srow, :] = tile_ref[
                8 - srow : 8, part * LANES : (part + 1) * LANES
            ]
    lower = lower_ones()
    heads = key_ref.shape[1] // DK
    spans = key_ref.shape[0] // BLK
    for head in range(heads):
        state = entry_ref[head * DV : (head + 1) * DV, :]
        for block in range(spans):
            log_cum, last = log_sums(decay_ref, head, block, lower)
            values = cut(value_ref, head, block, DV)
            keys = cut(key_ref, head, block, DK)
            q_dec = cut(query_ref, head, block, DK) * DK ** (-0.5) * jnp.exp(log_cum)
            k_grow = keys * jnp.exp(-log_cum)
            scores = dot_nt(q_dec, k_grow, HIGHEST_PREC) * lower
            out = dot_nt(q_dec, state, HIGHEST_PREC) + dot_nn(scores, values, HIGHEST_PREC)
            mixed_ref[
                block * BLK : (block + 1) * BLK, head * DV : (head + 1) * DV
            ] = out.astype(BF16)
            if block + 1 < spans:
                k_end = keys * jnp.exp(last - log_cum)
                state = jnp.exp(last) * state + dot_tn(values, k_end, HIGHEST_PREC)


def combine_kernel(stride, ids_ref, cot_ref, back_ref, out_ref):
    half = out_ref.shape[1]
    start = pl.multiple_of(lax.axis_index("tp") * half, LANES)
    slots = route_columns(ids_ref, stride)
    total = cot_ref[:, pl.ds(start, half)].astype(F32)
    width = back_ref.shape[0]
    chosen = one_hot(slots[0], 0, width) + one_hot(slots[1], 0, width)
    total = total + dot_nn(chosen, back_ref[...])
    out_ref[...] = total.astype(BF16)


def cotangent_kernel(
    groups, own_ref, other_ref, weight_ref, query_ref, decay_ref, cot_ref, back_ref, *rest
):
    sends, full_ref = rest[:-1], rest[-1]
    half = own_ref.shape[1]
    side = lax.axis_index("tp")
    full_ref[:, pl.ds(pl.multiple_of(side * half, LANES), half)] = own_ref[...]
    full_ref[:, pl.ds(pl.multiple_of((1 - side) * half, LANES), half)] = other_ref[...]
    cot_ref[...] = dot_nn(full_ref[...], weight_ref[...])
    lower = lower_ones()
    heads = query_ref.shape[1] // DK
    spans = query_ref.shape[0] // BLK
    for head in range(heads):
        state = None
        for block in reversed(range(spans)):
            log_cum, last = log_sums(decay_ref, head, block, lower)
            q_dec = cut(query_ref, head, block, DK) * DK ** (-0.5) * jnp.exp(log_cum)
            add = dot_tn(cut(cot_ref, head, block, DV), q_dec, HIGHEST_PREC)
            state = add if state is None else jnp.exp(last) * state + add
        back_ref[head * DV : (head + 1) * DV, :] = state.astype(BF16)
    member = lax.rem(lax.axis_index("sp"), GROUP)
    block_cols = full_ref.shape[1] // (GROUP * groups)
    for step, out_ref in enumerate(sends):
        peer = member ^ step
        for plane in range(groups):
            first = pl.multiple_of((plane * GROUP + peer) * block_cols, LANES)
            out_ref[:, plane * block_cols : (plane + 1) * block_cols] = full_ref[
                :, pl.ds(first, block_cols)
            ]


def plane_kernel(logs_ref, *refs):
    backs, suffix_ref, plane_ref = refs[:-2], refs[-2], refs[-1]
    logs = logs_ref[...]
    place = lax.axis_index("sp")
    member = lax.rem(place, GROUP)
    base = place - member
    heads = logs.shape[1] // DK
    after = None
    whole = None
    for step, back_ref in enumerate(backs):
        source = base + (member ^ step)
        later = jnp.where(source > place, 1.0, 0.0)
        tail = log_between(logs, place + 1, source) * later
        lead = log_between(logs, base, source)
        spread = [
            jnp.concatenate(
                [jnp.broadcast_to(c[:, h * DK : (h + 1) * DK], (DV, DK)) for h in range(heads)], axis=0
            )
            for c in (tail, lead)
        ]
        back = back_ref[...].astype(F32)
        after = spread[0] * back if after is None else after + spread[0] * back
        whole = spread[1] * back if whole is None else whole + spread[1] * back
    suffix_ref[...] = after
    plane_ref[...] = whole.astype(BF16)


def partial_kernel(groups, *refs):
    gts, mixes = refs[:GROUP], refs[GROUP : 2 * GROUP]
    outs, own_ref, total_ref = refs[2 * GROUP : -2], refs[-2], refs[-1]
    total = None
    for gt_ref, mix_ref in zip(gts, mixes):
        term = dot_tn(gt_ref[...], mix_ref[...])
        total = term if total is None else total + term
    total_ref[...] = total
    rows = own_ref.shape[0]
    plane = lax.div(lax.axis_index("sp"), GROUP)
    own_ref[...] = total_ref[pl.ds(pl.multiple_of(plane * rows, 8), rows), :]
    for step, out_ref in enumerate(outs):
        target = lax.rem(plane + step + 1, groups)
        out_ref[...] = total_ref[pl.ds(pl.multiple_of(target * rows, 8), rows), :].astype(BF16)


def final_kernel(
    groups, query_ref, key_ref, value_ref, decay_ref, cot_ref, entry_ref, logs_ref, suffix_ref, *refs
):
    planes = refs[: groups - 1]
    gq_ref, gk_ref, gv_ref, gd_ref, exit_ref = refs[groups - 1 :]
    logs = logs_ref[...]
    place = lax.axis_index("sp")
    base = place - lax.rem(place, GROUP)
    heads = key_ref.shape[1] // DK
    spans = key_ref.shape[0] // BLK

    def spread(c):
        return jnp.concatenate(
            [jnp.broadcast_to(c[:, h * DK : (h + 1) * DK], (DV, DK)) for h in range(heads)], axis=0
        )

    beyond = None
    for step, plane_ref in enumerate(planes):
        factor = spread(log_between(logs, base + GROUP, base + GROUP * (step + 1)))
        term = factor * plane_ref[...].astype(F32)
        beyond = term if beyond is None else beyond + term
    out = suffix_ref[...]
    if beyond is not None:
        out = out + spread(log_between(logs, place + 1, base + GROUP)) * beyond
    exit_ref[...] = out
    lower = lower_ones()
    for head in range(heads):
        state = entry_ref[head * DV : (head + 1) * DV, :]
        exit_cot = exit_ref[head * DV : (head + 1) * DV, :]
        parts = []
        for block in range(spans):
            log_cum, last = log_sums(decay_ref, head, block, lower)
            values = cut(value_ref, head, block, DV)
            keys = cut(key_ref, head, block, DK)
            grow_up = jnp.exp(log_cum)
            scaled_q = cut(query_ref, head, block, DK) * DK ** (-0.5)
            end_decay = jnp.exp(last - log_cum)
            parts.append((values, keys, grow_up, scaled_q, jnp.exp(-log_cum), end_decay, last, state))
            state = jnp.exp(last) * state + dot_tn(values, keys * end_decay, HIGHEST_PREC)
        running = jnp.sum(state * exit_cot, axis=0, keepdims=True)
        into = exit_cot
        for block in reversed(range(spans)):
            values, keys, grow_up, scaled_q, grow_down, end_decay, last, start = parts[block]
            cots = cut(cot_ref, head, block, DV)
            q_dec = scaled_q * grow_up
            k_grow = keys * grow_down
            k_end = keys * end_decay
            scores = dot_nt(q_dec, k_grow, HIGHEST_PREC) * lower
            cross = dot_nt(cots, values, HIGHEST_PREC) * lower
            grad_qs = grow_up * (
                dot_nn(cots, start, HIGHEST_PREC) + dot_nn(cross, k_grow, HIGHEST_PREC)
            )
            grad_k = grow_down * dot_tn(cross, q_dec, HIGHEST_PREC)
            grad_k = grad_k + end_decay * dot_nn(values, into, HIGHEST_PREC)
            grad_v = dot_tn(scores, cots, HIGHEST_PREC) + dot_nt(k_end, into, HIGHEST_PREC)
            log_grad = scaled_q * grad_qs - keys * grad_k
            suffix = dot_tn(lower, log_grad, HIGHEST_PREC) + running
            rows = slice(block * BLK, (block + 1) * BLK)
            narrow = slice(head * DK, (head + 1) * DK)
            gd_ref[rows, narrow] = suffix
            gq_ref[rows, narrow] = grad_qs * DK ** (-0.5)
            gk_ref[rows, narrow] = grad_k
            gv_ref[rows, head * DV : (head + 1) * DV] = grad_v
            running = suffix[0:1, :]
            if block:
                into = jnp.exp(last) * into + dot_tn(cots, q_dec, HIGHEST_PREC)


def expert_work(tok_rows, cot_rows, w_gate, w_up, w_down):
    pre_gate = dot_nn(tok_rows, w_gate)
    pre_up = dot_nn(tok_rows, w_up)
    gate_clamped = jnp.minimum(pre_gate, CLAMP_LIMIT)
    up_clamped = jnp.clip(pre_up, -CLAMP_LIMIT, CLAMP_LIMIT)
    sigmoid_gate = jax.nn.sigmoid(SWISH_ALPHA * gate_clamped)
    activated = ((up_clamped + 1.0) * gate_clamped * sigmoid_gate).astype(BF16)
    grad_down = dot_tn(activated, cot_rows).astype(BF16)
    grad_act = dot_nt(cot_rows, w_down)
    slope = (
        (up_clamped + 1.0)
        * sigmoid_gate
        * (1.0 + SWISH_ALPHA * gate_clamped * (1.0 - sigmoid_gate))
    )
    grad_pre_gate = jnp.where(pre_gate < CLAMP_LIMIT, grad_act * slope, 0.0).astype(BF16)
    grad_pre_up = jnp.where(
        jnp.abs(pre_up) < CLAMP_LIMIT, grad_act * gate_clamped * sigmoid_gate, 0.0
    ).astype(BF16)
    grad_wg = dot_tn(tok_rows, grad_pre_gate).astype(BF16)
    grad_wu = dot_tn(tok_rows, grad_pre_up).astype(BF16)
    piece_term = dot_nt(grad_pre_gate, w_gate) + dot_nt(grad_pre_up, w_up)
    return (grad_wg, grad_wu, grad_down, piece_term.astype(BF16))


def shards(
    moe_in,
    cotangent,
    route_ids,
    route_weights,
    gate_weight,
    up_weight,
    down_weight,
    out_weight,
    query,
    key_in,
    value,
    log_decay,
):
    count = lax.axis_size("sp")
    sides = lax.axis_size("tp")
    side = lax.axis_index("tp")
    tokens, width = moe_in.shape
    half = width // sides
    groups = count // GROUP
    heads = key_in.shape[1] // DK
    cap = tokens * TOP * 3 // (2 * count)
    state_rows = heads * DV
    srow = state_rows * DK // (count * half)
    stride = -(-(cap + srow) // 8) * 8
    slots = count * stride

    def exchange(rows):
        return lax.all_to_all(
            rows.reshape(count, stride, half), "sp", split_axis=0, concat_axis=0, tiled=True
        )

    def swap(array):
        return lax.ppermute(array, "tp", [(0, 1), (1, 0)])

    def member(array, step):
        return lax.ppermute(array, "sp", [(i, i ^ step) for i in range(count)])

    def both(own):
        other = swap(own)
        return jnp.where(
            side == 0,
            jnp.concatenate([own, other], axis=1),
            jnp.concatenate([other, own], axis=1),
        )

    send_tok, log_total = call(
        lambda *r: send_tokens_kernel(count, stride, srow, *r),
        (shape((slots, half), BF16), shape((1, heads * DK), F32)),
        [pltpu.VMEM((state_rows, DK), F32), pltpu.VMEM((8, half), F32)],
    )(route_ids, moe_in, key_in, value, log_decay)
    got_tok = exchange(send_tok)

    own_row = lax.broadcasted_iota(jnp.int32, (count, 1), 0) == lax.axis_index("sp")
    logs = jnp.where(own_row, log_total, 0.0)
    logs = sum((member(logs, step) for step in range(1, GROUP)), logs)
    logs = sum((member(logs, step * GROUP) for step in range(1, groups)), logs)

    send_cot = call(
        lambda *r: send_cots_kernel(count, stride, srow, *r), shape((slots, half), BF16)
    )(route_ids, route_weights, cotangent, got_tok[:, stride - 8 :, :], logs)
    got_cot = exchange(send_cot)

    tok_rows = both(got_tok.reshape(slots, half))
    live = lax.rem(lax.broadcasted_iota(jnp.int32, (slots, 1), 0), stride) < cap
    cot_rows = jnp.where(live, both(got_cot.reshape(slots, half)), 0.0).astype(BF16)

    mixed, entry = call(
        lambda *r: mixed_kernel(count, srow, *r),
        (shape((tokens, heads * DV), BF16), shape((state_rows, DK), F32)),
        [pltpu.VMEM((8, half), F32)],
    )(query, key_in, value, log_decay, got_cot[:, stride - 8 :, :])
    mixes = [mixed] + [member(mixed, step) for step in range(1, GROUP)]

    grad_wg, grad_wu, grad_down, pieces = expert_work(
        tok_rows, cot_rows, gate_weight[0], up_weight[0], down_weight[0]
    )
    mine = lax.dynamic_slice_in_dim(pieces, side * half, half, 1)
    theirs = swap(lax.dynamic_slice_in_dim(pieces, (1 - side) * half, half, 1))
    returned = exchange((mine.astype(F32) + theirs.astype(F32)).astype(BF16))

    grad_half = call(
        lambda *r: combine_kernel(stride, *r), shape((tokens, half), BF16)
    )(route_ids, cotangent, returned.reshape(slots, half))

    block_cols = width // GROUP
    outs = call(
        lambda *r: cotangent_kernel(groups, *r),
        (shape((tokens, heads * DV), F32), shape((state_rows, DK), BF16))
        + (shape((tokens, block_cols), BF16),) * GROUP,
        [pltpu.VMEM((tokens, width), BF16)],
    )(grad_half, swap(grad_half), out_weight, query, log_decay)
    mixer_cot, back, gts = outs[0], outs[1], outs[2:]

    backs = [back] + [member(back, step) for step in range(1, GROUP)]
    gts = [gts[0]] + [member(gts[step], step) for step in range(1, GROUP)]
    suffix, plane = call(
        plane_kernel, (shape((state_rows, DK), F32), shape((state_rows, DK), BF16))
    )(logs, *backs)
    planes = [
        lax.ppermute(
            plane, "sp", [(i + GROUP * step, i) for i in range(count - GROUP * step)]
        )
        for step in range(1, groups)
    ]
    rows = width // count
    outs = call(
        lambda *r: partial_kernel(groups, *r),
        (shape((rows, heads * DV), BF16),) * (groups - 1) + (shape((rows, heads * DV), F32),),
        [pltpu.VMEM((block_cols, heads * DV), F32)],
    )(*gts, *mixes)
    grad_out = outs[-1]
    for step in range(1, groups):
        grad_out = grad_out + lax.ppermute(
            outs[step - 1], "sp", [(i, (i + GROUP * step) % count) for i in range(count)]
        ).astype(F32)

    grad_query, grad_key, grad_value, grad_decay = call(
        lambda *r: final_kernel(groups, *r),
        (
            shape((tokens, heads * DK), F32),
            shape((tokens, heads * DK), F32),
            shape((tokens, heads * DV), F32),
            shape((tokens, heads * DK), F32),
        ),
        [pltpu.VMEM((state_rows, DK), F32)],
    )(query, key_in, value, log_decay, mixer_cot, entry, logs, suffix, *planes)
    return (
        grad_wg[None],
        grad_wu[None],
        grad_down[None],
        grad_out,
        grad_query,
        grad_key,
        grad_value,
        grad_decay,
    )


def solution(mesh):
    return jax.shard_map(
        shards,
        mesh=mesh,
        in_specs=(
            P("sp", None),
            P("sp", None),
            P("sp", None),
            P("sp", None),
            P("sp", None, "tp"),
            P("sp", None, "tp"),
            P("sp", "tp", None),
            P(None, "tp"),
            P("sp", "tp"),
            P("sp", "tp"),
            P("sp", "tp"),
            P("sp", "tp"),
        ),
        out_specs=(
            P("sp", None, "tp"),
            P("sp", None, "tp"),
            P("sp", "tp", None),
            P("sp", "tp"),
            P("sp", "tp"),
            P("sp", "tp"),
            P("sp", "tp"),
            P("sp", "tp"),
        ),
        check_vma=False,
    )
```
